32 devices in a mesh: sp: 8 (over z, x), tp: 4 (over y, core).
Axes of the slice: x: 2, y: 2, z: 4, core: 2. Of those that a mesh axis runs over, the one named last changes fastest.
Arguments:
- tokens: bfloat16 [6144, 2048], P('sp', 'tp'), may hold values from -23 to 23, as said below
- norm_gain: float32 [2048], replicated, may hold values from 0.8 to 8, as said below
- window_query: bfloat16 [2048, 1024], P(None, 'tp'), may hold values from -0.125 to 0.125
- window_key: bfloat16 [2048, 512], P(None, 'tp'), may hold values from -0.125 to 0.125
- window_value: bfloat16 [2048, 512], P(None, 'tp'), may hold values from -0.125 to 0.125
- sink_logit: float32 [16], P('tp'), may hold values from 2 to 6
- down_query: bfloat16 [2048, 768], replicated, may hold values from -0.125 to 0.125
- down_latent: bfloat16 [2048, 512], replicated, may hold values from -0.125 to 0.125
- rotary_proj: bfloat16 [2048, 32], replicated, may hold values from -0.125 to 0.125
- query_gain: float32 [768], replicated, may hold values from 0.8 to 8, as said below
- latent_gain: float32 [512], replicated, may hold values from 0.8 to 8, as said below
- up_query: bfloat16 [768, 1536], P(None, 'tp'), may hold values from -0.21875 to 0.21875
- up_key: bfloat16 [512, 1024], P(None, 'tp'), may hold values from -0.25 to 0.25
- up_value: bfloat16 [512, 1024], P(None, 'tp'), may hold values from -0.25 to 0.25
- window_out: bfloat16 [1024, 2048], P('tp'), may hold values from -0.125 to 0.125
- latent_out: bfloat16 [1024, 2048], P('tp'), may hold values from -0.125 to 0.125
Outputs:
- mixed: bfloat16 [6144, 2048], P(('sp', 'tp'))
The draws below stay inside these ranges and needn't reach their ends.
Inputs may be any that keep to these rules, and one draw needn't show every extreme that they name: `tokens`: real-valued; the channels carry scales that vary smoothly by a factor of up to twenty across the width. `norm_gain`: positive. `query_gain`: positive. `latent_gain`: positive.
All inputs are finite; a program needn't handle non-finite values.
Results may differ from the reference program's by a relative error of at most 0.04.
The reference program's roundings to bfloat16 on the way count: a program that leaves them out, or rounds other values in their place, can miss the bound.
Values may be sent and summed in bfloat16 or wider, within the bound.
A program may use at most 128 MiB of HBM per device.

```python
import jax
import jax.numpy as jnp
from jax import lax

D = 2048
A_HEADS = 16
KV_HEADS = 8
HD = 64
B_HEADS = 16
NOPE = 64
ROPE = 32
VD = 64
QRANK = 768
KVRANK = 512
WINDOW = 128
QBLOCK = 256
TOKENS = 6144
N_TP = 4


def gain_values(key, length):
    return jax.random.uniform(key, (length,), jnp.float32, 0.8, 2.4)


def draw_norm_gain(key, part):
    return gain_values(jax.random.fold_in(key, 11), D)


def draw_query_gain(key, part):
    return gain_values(jax.random.fold_in(key, 13), QRANK)


def draw_latent_gain(key, part):
    return gain_values(jax.random.fold_in(key, 17), KVRANK)


def draw_tokens(key, part):
    phase = jax.random.uniform(jax.random.fold_in(key, 3), (), jnp.float32, 0.0, 6.2831853)
    channel = jnp.arange(D, dtype=jnp.float32)
    channel_scale = jnp.exp(1.5 * jnp.cos(6.2831853 * channel / D + phase))
    base = jnp.clip(jax.random.normal(jax.random.fold_in(key, 7), (TOKENS, D), jnp.float32), -5.0, 5.0)
    return (base * channel_scale[None, :]).astype(jnp.bfloat16)


def block_scale(own_key, dims, pieces, low, top_value):
    gain, own = 1.0, jax.random.fold_in(own_key, 6)
    for axis_at, blocks in pieces:
        steps = jnp.exp(jax.random.uniform(jax.random.fold_in(own, axis_at), (blocks,), jnp.float32, low / len(pieces), top_value / len(pieces)))
        gain = gain * jnp.repeat(steps, dims[axis_at] // blocks).reshape([-1 if axis == axis_at else 1 for axis in range(len(dims))])
    return gain


def gaussian(key, extent, spread, reach, split=(), kind=jnp.bfloat16):
    array = jax.random.normal(key, extent, jnp.float32) * spread
    if len(split) > 0:
        array = block_scale(key, extent, split, -0.22, 0.18) * array
    return jnp.clip(array, min=-reach, max=reach).astype(kind)


def setup_inputs(seed: int = 0) -> dict:
    arg_keys = jax.random.split(jax.random.key(seed), 17)
    return {
        "tokens": draw_tokens(jax.random.fold_in(arg_keys[16], 71), 0),
        "norm_gain": draw_norm_gain(jax.random.fold_in(arg_keys[16], 71), 0),
        "window_query": gaussian(arg_keys[2], (D, A_HEADS * HD), D ** -0.5, 0.125, ((1, 4),)),
        "window_key": gaussian(arg_keys[3], (D, KV_HEADS * HD), D ** -0.5, 0.125, ((1, 4),)),
        "window_value": gaussian(arg_keys[4], (D, KV_HEADS * HD), D ** -0.5, 0.125, ((1, 4),)),
        "sink_logit": jnp.clip(2.0 + 4.0 * jax.random.uniform(arg_keys[5], (A_HEADS,), jnp.float32) ** block_scale(arg_keys[5], (A_HEADS,), ((0, 4),), -0.2, 0.2), 2.0, 6.0),
        "down_query": gaussian(arg_keys[6], (D, QRANK), D ** -0.5, 0.125),
        "down_latent": gaussian(arg_keys[7], (D, KVRANK), D ** -0.5, 0.125),
        "rotary_proj": gaussian(arg_keys[8], (D, ROPE), D ** -0.5, 0.125),
        "query_gain": draw_query_gain(jax.random.fold_in(arg_keys[16], 71), 0),
        "latent_gain": draw_latent_gain(jax.random.fold_in(arg_keys[16], 71), 0),
        "up_query": gaussian(arg_keys[11], (QRANK, B_HEADS * (NOPE + ROPE)), QRANK ** -0.5, 0.21875, ((1, 4),)),
        "up_key": gaussian(arg_keys[12], (KVRANK, B_HEADS * NOPE), KVRANK ** -0.5, 0.25, ((1, 4),)),
        "up_value": gaussian(arg_keys[13], (KVRANK, B_HEADS * VD), KVRANK ** -0.5, 0.25, ((1, 4),)),
        "window_out": gaussian(arg_keys[14], (A_HEADS * HD, D), (A_HEADS * HD + B_HEADS * VD) ** -0.5, 0.125, ((0, 4),)),
        "latent_out": gaussian(arg_keys[15], (B_HEADS * VD, D), (A_HEADS * HD + B_HEADS * VD) ** -0.5, 0.125, ((0, 4),)),
    }


EPS = 1e-06
THETA = 10000.0

def rotate(vector, positions):
    half_len = vector.shape[-1] // 2
    inverse = THETA ** (-jnp.arange(half_len, dtype=jnp.float32) / half_len)
    angles = positions.astype(jnp.float32)[:, None] * inverse[None, :]
    new_shape = (angles.shape[0],) + (1,) * (vector.ndim - 2) + (half_len,)
    cosine = jnp.cos(angles).reshape(new_shape)
    sine_part = jnp.sin(angles).reshape(new_shape)
    front_half = vector[..., :half_len].astype(jnp.float32)
    second = vector[..., half_len:].astype(jnp.float32)
    return jnp.concatenate([front_half * cosine - second * sine_part, second * cosine + front_half * sine_part], axis=-1)

def norm_rows(values, gain_vec):
    as_float = values.astype(jnp.float32)
    return (as_float * lax.rsqrt(lax.optimization_barrier(jnp.mean(as_float * as_float, axis=1, keepdims=True)) + EPS) * gain_vec).astype(jnp.bfloat16)

def window_attention(q_rows, key_rows, value_rows, sink_logit):
    row_count = q_rows.shape[0]
    group = A_HEADS // KV_HEADS
    padded_keys = jnp.pad(key_rows, ((WINDOW, WINDOW), (0, 0)))
    padded_values = jnp.pad(value_rows, ((WINDOW, WINDOW), (0, 0)))
    span_len = QBLOCK + 2 * WINDOW
    distance = jnp.arange(QBLOCK)[:, None] + WINDOW - jnp.arange(span_len)[None, :]
    slopes = jnp.exp2(-8.0 * (jnp.arange(A_HEADS, dtype=jnp.float32) + 1.0) / A_HEADS).reshape(KV_HEADS, group)
    sinks = sink_logit.astype(jnp.float32).reshape(KV_HEADS, group)[:, :, None, None]

    def one_block(offset):
        queries = lax.dynamic_slice_in_dim(q_rows, offset, QBLOCK, 0).astype(jnp.float32).reshape(QBLOCK, KV_HEADS, group, HD)
        key_part = lax.dynamic_slice_in_dim(padded_keys, offset, span_len, 0).astype(jnp.float32).reshape(span_len, KV_HEADS, HD)
        value_part = lax.dynamic_slice_in_dim(padded_values, offset, span_len, 0).astype(jnp.float32).reshape(span_len, KV_HEADS, HD)
        scores = jnp.einsum('qhgd,khd->hgqk', queries, key_part) * HD ** (-0.5)
        scores = scores - slopes[:, :, None, None] * jnp.abs(distance).astype(jnp.float32)
        key_pos = offset + jnp.arange(span_len, dtype=jnp.int32) - WINDOW
        valid = (jnp.abs(distance) <= WINDOW) & ((key_pos >= 0) & (key_pos < row_count))[None, :]
        scores = jnp.where(valid, scores, -jnp.inf)
        row_max = jnp.maximum(lax.optimization_barrier(jnp.max(scores, axis=3, keepdims=True)), sinks)
        weights = jnp.exp(scores - row_max)
        weights = weights / (lax.optimization_barrier(jnp.sum(weights, axis=3, keepdims=True)) + jnp.exp(sinks - row_max))
        rounded = lax.optimization_barrier(weights.astype(jnp.bfloat16)).astype(jnp.float32)
        return jnp.einsum('hgqk,khd->qhgd', rounded, value_part).astype(jnp.bfloat16).reshape(QBLOCK, A_HEADS * HD)
    offsets = (jnp.arange(row_count // QBLOCK) * QBLOCK).astype(jnp.int32)
    return lax.map(one_block, offsets).reshape(row_count, A_HEADS * HD)

def latent_attention(q_nope, q_rot, key_rows, value_rows, k_rot):
    row_count = q_nope.shape[0]
    lat_scale = (NOPE + ROPE) ** (-0.5)
    keys_float = key_rows.astype(jnp.float32)
    values_float = value_rows.astype(jnp.float32)
    krot_float = k_rot.astype(jnp.float32)

    def one_block(offset):
        q_part = lax.dynamic_slice_in_dim(q_nope, offset, QBLOCK, 0).astype(jnp.float32)
        rot_part = lax.dynamic_slice_in_dim(q_rot, offset, QBLOCK, 0).astype(jnp.float32)
        scores = (jnp.einsum('qhd,khd->hqk', q_part, keys_float) + jnp.einsum('qhr,kr->hqk', rot_part, krot_float)) * lat_scale
        row_max = lax.optimization_barrier(jnp.max(scores, axis=2, keepdims=True))
        weights = jnp.exp(scores - row_max)
        denom_sum = lax.optimization_barrier(jnp.sum(weights, axis=2))
        rounded = lax.optimization_barrier(weights.astype(jnp.bfloat16)).astype(jnp.float32)
        summed = jnp.einsum('hqk,khd->qhd', rounded, values_float)
        return (summed / denom_sum.T[:, :, None]).astype(jnp.bfloat16)
    offsets = (jnp.arange(row_count // QBLOCK) * QBLOCK).astype(jnp.int32)
    return lax.map(one_block, offsets).reshape(row_count, B_HEADS * VD)

def reference(tokens, norm_gain, window_query, window_key, window_value, sink_logit, down_query, down_latent, rotary_proj, query_gain, latent_gain, up_query, up_key, up_value, window_out, latent_out):
    row_count = tokens.shape[0]
    as_float = tokens.astype(jnp.float32)
    row_scale = lax.rsqrt(lax.optimization_barrier(jnp.mean(as_float * as_float, axis=1, keepdims=True)) + EPS)
    scaled = (as_float * norm_gain).astype(jnp.bfloat16)

    def project(weight):
        return (jnp.dot(scaled, weight, preferred_element_type=jnp.float32) * row_scale).astype(jnp.bfloat16)
    q_window = project(window_query)
    k_window = project(window_key)
    v_window = project(window_value)
    latent_q = project(down_query)
    latent_kv = project(down_latent)
    rotary_rows = project(rotary_proj)
    positions = jnp.arange(row_count, dtype=jnp.int32)
    out_window = window_attention(q_window, k_window, v_window, sink_logit)
    q_latent = jnp.dot(norm_rows(latent_q, query_gain), up_query, preferred_element_type=jnp.float32).astype(jnp.bfloat16)
    q_latent = q_latent.reshape(row_count, B_HEADS, NOPE + ROPE)
    normed_kv = norm_rows(latent_kv, latent_gain)
    key_rows = jnp.dot(normed_kv, up_key, preferred_element_type=jnp.float32).astype(jnp.bfloat16).reshape(row_count, B_HEADS, NOPE)
    value_rows = jnp.dot(normed_kv, up_value, preferred_element_type=jnp.float32).astype(jnp.bfloat16).reshape(row_count, B_HEADS, VD)
    q_nope = q_latent[..., :NOPE]
    q_rot = rotate(q_latent[..., NOPE:], positions).astype(jnp.bfloat16)
    k_rot = rotate(rotary_rows, positions).astype(jnp.bfloat16)
    out_latent = latent_attention(q_nope, q_rot, key_rows, value_rows, k_rot)
    a_share = A_HEADS * HD // N_TP
    b_share = B_HEADS * VD // N_TP
    summed = jnp.zeros((row_count, D), jnp.float32)
    for member in range(N_TP):
        head_part = jnp.dot(out_window[:, member * a_share:(member + 1) * a_share], window_out[member * a_share:(member + 1) * a_share], preferred_element_type=jnp.float32)
        head_part = head_part + jnp.dot(out_latent[:, member * b_share:(member + 1) * b_share], latent_out[member * b_share:(member + 1) * b_share], preferred_element_type=jnp.float32)
        summed = summed + lax.optimization_barrier(head_part.astype(jnp.bfloat16)).astype(jnp.float32)
    return summed.astype(jnp.bfloat16)
```

```python
import functools

import jax
import jax.numpy as jnp
from jax import lax
from jax.experimental import pallas as pl
from jax.experimental.pallas import tpu as pltpu
from jax.sharding import PartitionSpec as P

A_HEADS = 16
HD = 64
NOPE = 64
ROPE = 32
VD = 64
WINDOW = 128
QBLOCK = 256
EPS = 1e-06
THETA = 10000.0
LANES = 128
LOG2E = 1.4426950408889634
VMEM_LIMIT = 60 * 1024 * 1024
BF = jnp.bfloat16
F32 = jnp.float32


def vmem():
    return pl.BlockSpec(memory_space=pltpu.VMEM)


def fdot(a, b):
    return jnp.dot(a, b, preferred_element_type=F32)


def fdot_t(a, b):
    return lax.dot_general(a, b, (((1,), (1,)), ((), ())), preferred_element_type=F32)


def normed(values, gain):
    v = values.astype(F32)
    return (v * lax.rsqrt(jnp.mean(v * v, axis=1, keepdims=True) + EPS) * gain).astype(BF)


def rotated(rope, cos, sin):
    half = ROPE // 2
    swapped = jnp.concatenate([rope[:, half:], rope[:, :half]], axis=1)
    return (rope * cos + swapped * sin).astype(BF)


def project_kernel(x, gain, wq, wk, wv, dq, dl, rp, qg, lg, uq, cs, sn,
                   qw_out, kv_out, q_out, g_out, *, block, heads, tp):
    rows = x.shape[0]
    own = rows // tp
    kvr = dl.shape[1]
    kcols = wk.shape[1]
    gain_row = gain[...]

    def scaled_rows(xs):
        xf = xs.astype(F32)
        rs = lax.rsqrt(jnp.mean(xf * xf, axis=1, keepdims=True) + EPS)
        return (xf * gain_row).astype(BF), rs

    start = pl.multiple_of(lax.axis_index("tp") * own, 16)
    mine = pl.ds(start, own)
    sc, rs = scaled_rows(x[mine, :])
    g_out[:, :kvr] = normed((fdot(sc, dl[...]) * rs).astype(BF), lg[...])
    rot = (fdot(sc, rp[...]) * rs).astype(BF).astype(F32)
    g_out[:, kvr:kvr + ROPE] = rotated(rot, cs[mine, :], sn[mine, :])
    g_out[:, kvr + ROPE:] = jnp.zeros((own, g_out.shape[1] - kvr - ROPE), BF)

    @pl.loop(0, rows // block)
    def _(i):
        at = pl.ds(pl.multiple_of(i * block, block), block)
        sc, rs = scaled_rows(x[at, :])
        qw_out[at, :] = (fdot(sc, wq[...]) * rs).astype(BF)
        kv_out[at, :kcols] = (fdot(sc, wk[...]) * rs).astype(BF)
        kv_out[at, kcols:] = (fdot(sc, wv[...]) * rs).astype(BF)
        nq = normed((fdot(sc, dq[...]) * rs).astype(BF), qg[...])
        ql = fdot(nq, uq[...]).astype(BF).astype(F32)
        cos, sin = cs[at, :], sn[at, :]
        for h in range(heads):
            base = h * (NOPE + ROPE)
            q_out[h, at, :NOPE] = ql[:, base:base + NOPE].astype(BF)
            q_out[h, at, NOPE:NOPE + ROPE] = rotated(
                ql[:, base + NOPE:base + NOPE + ROPE], cos, sin)
            q_out[h, at, NOPE + ROPE:] = jnp.zeros((block, LANES - NOPE - ROPE), BF)


def window_kernel(q, kv, before, after, sink, slope, out, pad, *, kv_dev, group, sp):
    rows = q.shape[0]
    me = lax.axis_index("sp")
    kcols = kv_dev * HD
    pad[:WINDOW, :] = before[...]
    pad[WINDOW:WINDOW + rows, :] = kv[...]
    pad[WINDOW + rows:, :] = after[...]
    span = QBLOCK + 2 * WINDOW
    dist = jnp.abs(
        lax.broadcasted_iota(jnp.int32, (QBLOCK, span), 0) + WINDOW
        - lax.broadcasted_iota(jnp.int32, (QBLOCK, span), 1))
    distf = dist.astype(F32)
    col = lax.broadcasted_iota(jnp.int32, (QBLOCK, span), 1)

    @pl.loop(0, rows // QBLOCK)
    def _(b):
        at = pl.multiple_of(b * QBLOCK, QBLOCK)
        pos = me * rows + at - WINDOW + col
        valid = (dist <= WINDOW) & (pos >= 0) & (pos < rows * sp)
        for g in range(kv_dev):
            keys = pad[pl.ds(at, span), g * HD:(g + 1) * HD]
            vals = pad[pl.ds(at, span), kcols + g * HD:kcols + (g + 1) * HD]
            for j in range(group):
                h = g * group + j
                s = fdot_t(q[pl.ds(at, QBLOCK), h * HD:(h + 1) * HD], keys) * HD ** (-0.5)
                s = jnp.where(valid, s - slope[0, h] * distf, -jnp.inf)
                snk = sink[0, h]
                m = jnp.maximum(jnp.max(s, axis=1, keepdims=True), snk)
                e = jnp.exp(s - m)
                w = e / (jnp.sum(e, axis=1, keepdims=True) + jnp.exp(snk - m))
                out[pl.ds(at, QBLOCK), h * HD:(h + 1) * HD] = fdot(w.astype(BF), vals).astype(BF)


def latent_kernel(q, g, ukv, out, ks, vs, s0, s1, *, heads, qb, kc, eb):
    rows = q.shape[1]
    total = g.shape[0]
    kvr = ukv.shape[0]
    kcols = heads * NOPE
    nq = rows // qb
    steps = heads * nq
    mult = LOG2E * (NOPE + ROPE) ** (-0.5)

    @pl.loop(0, total // eb)
    def _(c):
        at = pl.ds(pl.multiple_of(c * eb, eb), eb)
        both = fdot(g[at, :kvr], ukv[...]).astype(BF)
        tail = g[at, kvr:kvr + LANES - NOPE]
        lane = lax.broadcasted_iota(jnp.int32, (eb, LANES - VD), 1)
        one = jnp.where(lane == 0, 1.0, 0.0).astype(BF)
        for h in range(heads):
            ks[h, at, :NOPE] = both[:, h * NOPE:(h + 1) * NOPE]
            ks[h, at, NOPE:] = tail
            vs[h, at, :VD] = both[:, kcols + h * VD:kcols + (h + 1) * VD]
            vs[h, at, VD:] = one

    def q_of(i):
        return q[i // nq, pl.ds(pl.multiple_of(lax.rem(i, nq) * qb, qb), qb), :]

    def score(i, dst, c, top):
        at = slice(c * kc, (c + 1) * kc)
        s = fdot_t(q_of(i), ks[i // nq, at, :])
        dst[:, at] = s
        for j in range(kc // LANES):
            part = s[:, j * LANES:(j + 1) * LANES]
            top = part if top is None else jnp.maximum(top, part)
        return top

    def fold(i, src, c, shift, acc):
        at = slice(c * kc, (c + 1) * kc)
        p = jnp.exp2(src[:, at] * mult - shift).astype(BF)
        o = fdot(p, vs[i // nq, at, :])
        return o if acc is None else acc + o

    def finish(i, acc):
        h = i // nq
        res = (acc[:, :VD] / acc[:, VD:VD + 1]).astype(BF)
        out[h, pl.ds(pl.multiple_of(lax.rem(i, nq) * qb, qb), qb), :] = res

    def shift_of(top):
        return jnp.max(top, axis=1, keepdims=True) * mult

    chunks = total // kc
    top = None
    for c in range(chunks):
        top = score(0, s0, c, top)

    def pair(i, shift):
        for cur, nxt in ((s0, s1), (s1, s0)):
            top, acc = None, None
            following = jnp.minimum(i + 1, steps - 1)
            for c in range(chunks):
                top = score(following, nxt, c, top)
                acc = fold(i, cur, c, shift, acc)
            finish(i, acc)
            shift = shift_of(top)
            i = i + 1
        return shift

    lax.fori_loop(0, steps // 2, lambda t, s: pair(2 * t, s), shift_of(top))


def per_device(tokens, norm_gain, window_query, window_key, window_value, sink_logit, down_query,
               down_latent, rotary_proj, query_gain, latent_gain, up_query, up_key, up_value,
               window_out, latent_out):
    rows = tokens.shape[0]
    sp, tp = lax.axis_size("sp"), lax.axis_size("tp")
    heads = up_query.shape[1] // (NOPE + ROPE)
    heads_dev = window_query.shape[1] // HD
    kv_dev = window_key.shape[1] // HD
    group = heads_dev // kv_dev
    kvr = down_latent.shape[1]
    gw = kvr + LANES
    own = rows // tp
    seq = lax.axis_index("sp")
    half = ROPE // 2
    inverse = THETA ** (-jnp.arange(half, dtype=F32) / half)
    angles = (seq * rows + jnp.arange(rows, dtype=jnp.int32)).astype(F32)[:, None] * inverse[None]
    c, s = jnp.cos(angles), jnp.sin(angles)
    cs, sn = jnp.concatenate([c, c], 1), jnp.concatenate([-s, s], 1)

    x = lax.all_gather(tokens, "tp", axis=1, tiled=True)
    qw, kv, q, g = pl.pallas_call(
        functools.partial(project_kernel, block=256, heads=heads, tp=tp),
        out_shape=(
            jax.ShapeDtypeStruct((rows, heads_dev * HD), BF),
            jax.ShapeDtypeStruct((rows, 2 * kv_dev * HD), BF),
            jax.ShapeDtypeStruct((heads, rows, LANES), BF),
            jax.ShapeDtypeStruct((own, gw), BF),
        ),
        in_specs=[vmem()] * 13,
        out_specs=[vmem()] * 4,
        compiler_params=pltpu.CompilerParams(vmem_limit_bytes=VMEM_LIMIT),
        name="project",
    )(x, norm_gain[None], window_query, window_key, window_value, down_query, down_latent,
      rotary_proj, query_gain[None], latent_gain[None], up_query, cs, sn)

    g_all = lax.all_gather(g, ("sp", "tp"), axis=0, tiled=True)
    up = [(i, i + 1) for i in range(sp - 1)]
    before = lax.ppermute(kv[rows - WINDOW:], "sp", up)
    after = lax.ppermute(kv[:WINDOW], "sp", [(j, i) for i, j in up])

    ids = lax.axis_index("tp") * heads_dev + jnp.arange(heads_dev, dtype=jnp.int32)
    slopes = jnp.exp2(-8.0 * (ids.astype(F32) + 1.0) / A_HEADS)[None]
    smem = pl.BlockSpec(memory_space=pltpu.SMEM)
    out_window = pl.pallas_call(
        functools.partial(window_kernel, kv_dev=kv_dev, group=group, sp=sp),
        out_shape=jax.ShapeDtypeStruct((rows, heads_dev * HD), BF),
        in_specs=[vmem()] * 4 + [smem] * 2,
        out_specs=vmem(),
        scratch_shapes=[pltpu.VMEM((rows + 2 * WINDOW, 2 * kv_dev * HD), BF)],
        compiler_params=pltpu.CompilerParams(vmem_limit_bytes=VMEM_LIMIT),
        cost_estimate=pl.CostEstimate(flops=2 * 10**9, bytes_accessed=2**21, transcendentals=2**21),
        name="window",
    )(qw, kv, before, after, sink_logit[None], slopes)

    total = rows * sp
    ukv = jnp.concatenate([up_key, up_value], axis=1)
    out_latent = pl.pallas_call(
        functools.partial(latent_kernel, heads=heads, qb=256, kc=1024, eb=512),
        out_shape=jax.ShapeDtypeStruct((heads, rows, VD), BF),
        in_specs=[vmem()] * 3,
        out_specs=vmem(),
        scratch_shapes=[
            pltpu.VMEM((heads, total, LANES), BF),
            pltpu.VMEM((heads, total, LANES), BF),
            pltpu.VMEM((256, total), F32),
            pltpu.VMEM((256, total), F32),
        ],
        compiler_params=pltpu.CompilerParams(vmem_limit_bytes=VMEM_LIMIT),
        name="latent",
    )(q, g_all, ukv)
    out_latent = out_latent.transpose(1, 0, 2).reshape(rows, heads * VD)
    share = (fdot(out_window, window_out) + fdot(out_latent, latent_out)).astype(BF)
    return lax.psum_scatter(share, "tp", scatter_dimension=0, tiled=True)


def solution(mesh):
    placed = (
        P("sp", "tp"), P(), P(None, "tp"), P(None, "tp"), P(None, "tp"), P("tp"), P(), P(), P(),
        P(), P(), P(None, "tp"), P(None, "tp"), P(None, "tp"), P("tp", None), P("tp", None),
    )
    return jax.shard_map(
        per_device, mesh=mesh, in_specs=placed, out_specs=P(("sp", "tp"), None), check_vma=False
    )
```

```python
import functools

import jax
import jax.numpy as jnp
from jax import lax
from jax.experimental import pallas as pl
from jax.experimental.pallas import tpu as pltpu
from jax.sharding import PartitionSpec as P

A_HEADS = 16
HD = 64
NOPE = 64
ROPE = 32
VD = 64
WINDOW = 128
QBLOCK = 256
EPS = 1e-06
THETA = 10000.0
LANES = 128
LOG2E = 1.4426950408889634
VMEM_LIMIT = 60 * 1024 * 1024
BF = jnp.bfloat16
F32 = jnp.float32


def vmem():
    return pl.BlockSpec(memory_space=pltpu.VMEM)


def fdot(a, b):
    return jnp.dot(a, b, preferred_element_type=F32)


def fdot_t(a, b):
    return lax.dot_general(a, b, (((1,), (1,)), ((), ())), preferred_element_type=F32)


def normed(values, gain):
    v = values.astype(F32)
    return (v * lax.rsqrt(jnp.mean(v * v, axis=1, keepdims=True) + EPS) * gain).astype(BF)


def rotated(rope, cos, sin):
    half = ROPE // 2
    swapped = jnp.concatenate([rope[:, half:], rope[:, :half]], axis=1)
    return (rope * cos + swapped * sin).astype(BF)


def scaled_rows(xs, gain_row):
    xf = xs.astype(F32)
    rs = lax.rsqrt(jnp.mean(xf * xf, axis=1, keepdims=True) + EPS)
    return (xf * gain_row).astype(BF), rs


def compress_kernel(x, gain, dl, rp, lg, cs, sn, g0_out, g1_out):
    kvr = dl.shape[1]
    half = g0_out.shape[0]
    sc, rs = scaled_rows(x[...], gain[...])
    nkv = normed((fdot(sc, dl[...]) * rs).astype(BF), lg[...])
    rot = (fdot(sc, rp[...]) * rs).astype(BF).astype(F32)
    rot = rotated(rot, cs[...], sn[...])
    for k, ref in enumerate((g0_out, g1_out)):
        at = slice(k * half, (k + 1) * half)
        ref[:, :kvr] = nkv[at, :]
        ref[:, kvr:kvr + ROPE] = rot[at, :]
        ref[:, kvr + ROPE:] = jnp.zeros((half, ref.shape[1] - kvr - ROPE), BF)


def project_kernel(x, gain, wq, wk, wv, dq, qg, uq, cs, sn, qw_out, kv_out, q_out, *, block, heads):
    rows = x.shape[0]
    kcols = wk.shape[1]
    gain_row = gain[...]

    @pl.loop(0, rows // block)
    def _(i):
        at = pl.ds(pl.multiple_of(i * block, block), block)
        sc, rs = scaled_rows(x[at, :], gain_row)
        qw_out[at, :] = (fdot(sc, wq[...]) * rs).astype(BF)
        kv_out[at, :kcols] = (fdot(sc, wk[...]) * rs).astype(BF)
        kv_out[at, kcols:] = (fdot(sc, wv[...]) * rs).astype(BF)
        nq = normed((fdot(sc, dq[...]) * rs).astype(BF), qg[...])
        ql = fdot(nq, uq[...]).astype(BF).astype(F32)
        cos, sin = cs[at, :], sn[at, :]
        for h in range(heads):
            base = h * (NOPE + ROPE)
            q_out[h, at, :NOPE] = ql[:, base:base + NOPE].astype(BF)
            q_out[h, at, NOPE:NOPE + ROPE] = rotated(
                ql[:, base + NOPE:base + NOPE + ROPE], cos, sin)
            q_out[h, at, NOPE + ROPE:] = jnp.zeros((block, LANES - NOPE - ROPE), BF)


def window_kernel(q, kv, before, after, sink, slope, out, pad, *, kv_dev, group, sp):
    rows = q.shape[0]
    me = lax.axis_index("sp")
    kcols = kv_dev * HD
    pad[:WINDOW, :] = before[...]
    pad[WINDOW:WINDOW + rows, :] = kv[...]
    pad[WINDOW + rows:, :] = after[...]
    span = QBLOCK + 2 * WINDOW
    dist = jnp.abs(
        lax.broadcasted_iota(jnp.int32, (QBLOCK, span), 0) + WINDOW
        - lax.broadcasted_iota(jnp.int32, (QBLOCK, span), 1))
    distf = dist.astype(F32)
    col = lax.broadcasted_iota(jnp.int32, (QBLOCK, span), 1)

    @pl.loop(0, rows // QBLOCK)
    def _(b):
        at = pl.multiple_of(b * QBLOCK, QBLOCK)
        pos = me * rows + at - WINDOW + col
        valid = (dist <= WINDOW) & (pos >= 0) & (pos < rows * sp)
        for g in range(kv_dev):
            keys = pad[pl.ds(at, span), g * HD:(g + 1) * HD]
            vals = pad[pl.ds(at, span), kcols + g * HD:kcols + (g + 1) * HD]
            for j in range(group):
                h = g * group + j
                s = fdot_t(q[pl.ds(at, QBLOCK), h * HD:(h + 1) * HD], keys) * HD ** (-0.5)
                s = jnp.where(valid, s - slope[0, h] * distf, -jnp.inf)
                snk = sink[0, h]
                m = jnp.maximum(jnp.max(s, axis=1, keepdims=True), snk)
                e = jnp.exp(s - m)
                w = e / (jnp.sum(e, axis=1, keepdims=True) + jnp.exp(snk - m))
                out[pl.ds(at, QBLOCK), h * HD:(h + 1) * HD] = fdot(w.astype(BF), vals).astype(BF)


def latent_kernel(*refs, heads, qb, kc, eb, last):
    if last:
        q, g, ukv, earlier, out, ks, vs, s0, s1 = refs
    else:
        q, g, ukv, out, ks, vs, s0, s1 = refs
    rows = q.shape[1]
    total = g.shape[0]
    kvr = ukv.shape[0]
    kcols = heads * NOPE
    nq = rows // qb
    steps = heads * nq
    mult = LOG2E * (NOPE + ROPE) ** (-0.5)

    @pl.loop(0, total // eb)
    def _(c):
        at = pl.ds(pl.multiple_of(c * eb, eb), eb)
        both = fdot(g[at, :kvr], ukv[...]).astype(BF)
        tail = g[at, kvr:kvr + LANES - NOPE]
        lane = lax.broadcasted_iota(jnp.int32, (eb, LANES - VD), 1)
        one = jnp.where(lane == 0, 1.0, 0.0).astype(BF)
        for h in range(heads):
            ks[h, at, :NOPE] = both[:, h * NOPE:(h + 1) * NOPE]
            ks[h, at, NOPE:] = tail
            vs[h, at, :VD] = both[:, kcols + h * VD:kcols + (h + 1) * VD]
            vs[h, at, VD:] = one

    def q_of(i):
        return q[i // nq, pl.ds(pl.multiple_of(lax.rem(i, nq) * qb, qb), qb), :]

    def score(i, dst, c, top):
        at = slice(c * kc, (c + 1) * kc)
        s = fdot_t(q_of(i), ks[i // nq, at, :])
        dst[:, at] = s
        for j in range(kc // LANES):
            part = s[:, j * LANES:(j + 1) * LANES]
            top = part if top is None else jnp.maximum(top, part)
        return top

    def fold(i, src, c, shift, acc):
        at = slice(c * kc, (c + 1) * kc)
        p = jnp.exp2(src[:, at] * mult - shift).astype(BF)
        o = fdot(p, vs[i // nq, at, :])
        return o if acc is None else acc + o

    def finish(i, acc, shift):
        h = i // nq
        at = pl.ds(pl.multiple_of(lax.rem(i, nq) * qb, qb), qb)
        if last:
            was = earlier[h, at, :]
            was_shift = was[:, VD + 1:VD + 2]
            top = jnp.maximum(shift, was_shift)
            acc = acc * jnp.exp2(shift - top) + was * jnp.exp2(was_shift - top)
            out[h, at, :] = (acc[:, :VD] / acc[:, VD:VD + 1]).astype(BF)
        else:
            lane = lax.broadcasted_iota(jnp.int32, acc.shape, 1)
            out[h, at, :] = jnp.where(lane == VD + 1, shift, acc)

    def shift_of(top):
        return jnp.max(top, axis=1, keepdims=True) * mult

    chunks = total // kc
    top = None
    for c in range(chunks):
        top = score(0, s0, c, top)

    def pair(i, shift):
        for cur, nxt in ((s0, s1), (s1, s0)):
            top, acc = None, None
            following = jnp.minimum(i + 1, steps - 1)
            for c in range(chunks):
                top = score(following, nxt, c, top)
                acc = fold(i, cur, c, shift, acc)
            finish(i, acc, shift)
            shift = shift_of(top)
            i = i + 1
        return shift

    lax.fori_loop(0, steps // 2, lambda t, s: pair(2 * t, s), shift_of(top))


def mix_kernel(ow, ol, wa, wb, out, to_pair, from_pair, to_far, from_far,
               pair_send, pair_recv, far_send, far_recv, *, chips, own):
    me = lax.axis_index("tp")
    chip, core = me // 2, lax.rem(me, 2)
    pair = chip * 2 + 1 - core
    mesh = pl.DeviceIdType.MESH

    def chip_at(step):
        return lax.rem(chip + step, chips)

    def share(dest):
        at = pl.ds(pl.multiple_of(dest * own, 16), own)
        return (fdot(ow[at, :], wa[...]) + fdot(ol[at, :], wb[...])).astype(BF)

    barrier = pltpu.get_barrier_semaphore()
    pl.semaphore_signal(barrier, inc=1, device_id={"tp": pair}, device_id_type=mesh)
    for step in range(1, chips):
        pl.semaphore_signal(barrier, inc=1, device_id={"tp": chip_at(step) * 2 + core},
                            device_id_type=mesh)
    pl.semaphore_wait(barrier, chips)

    order = list(range(1, chips)) + [0]
    copies = []
    for step in order:
        to_pair[step] = share(chip_at(step) * 2 + 1 - core)
        copy = pltpu.make_async_remote_copy(
            to_pair.at[step], from_pair.at[step], pair_send.at[step], pair_recv.at[step],
            device_id={"tp": pair}, device_id_type=mesh)
        copy.start()
        copies.append(copy)
    far = []
    for k, step in enumerate(order[:-1]):
        mine = share(chip_at(step) * 2 + core).astype(F32)
        copies[k].wait_recv()
        to_far[step - 1] = (mine + from_pair[step].astype(F32)).astype(BF)
        copy = pltpu.make_async_remote_copy(
            to_far.at[step - 1], from_far.at[step - 1], far_send.at[step - 1],
            far_recv.at[step - 1],
            device_id={"tp": chip_at(step) * 2 + core}, device_id_type=mesh)
        copy.start()
        far.append(copy)
    total = share(me).astype(F32)
    copies[-1].wait_recv()
    total = total + from_pair[0].astype(F32)
    for k, copy in enumerate(far):
        copy.wait_recv()
        total = total + from_far[k].astype(F32)
    out[...] = total.astype(BF)
    for copy in copies + far:
        copy.wait_send()


def per_device(tokens, norm_gain, window_query, window_key, window_value, sink_logit, down_query,
               down_latent, rotary_proj, query_gain, latent_gain, up_query, up_key, up_value,
               window_out, latent_out):
    rows = tokens.shape[0]
    sp, tp = lax.axis_size("sp"), lax.axis_size("tp")
    heads = up_query.shape[1] // (NOPE + ROPE)
    heads_dev = window_query.shape[1] // HD
    kv_dev = window_key.shape[1] // HD
    group = heads_dev // kv_dev
    kvr = down_latent.shape[1]
    gw = kvr + LANES
    own = rows // tp
    seq = lax.axis_index("sp")
    half = ROPE // 2
    inverse = THETA ** (-jnp.arange(half, dtype=F32) / half)
    angles = (seq * rows + jnp.arange(rows, dtype=jnp.int32)).astype(F32)[:, None] * inverse[None]
    c, s = jnp.cos(angles), jnp.sin(angles)
    cs, sn = jnp.concatenate([c, c], 1), jnp.concatenate([-s, s], 1)

    x = lax.all_gather(tokens, "tp", axis=1, tiled=True)
    params = pltpu.CompilerParams(vmem_limit_bytes=VMEM_LIMIT)
    first = lax.axis_index("tp") * own
    take = lambda arr: lax.dynamic_slice_in_dim(arr, first, own, 0)
    g0, g1 = pl.pallas_call(
        compress_kernel,
        out_shape=(jax.ShapeDtypeStruct((own // 2, gw), BF),) * 2,
        in_specs=[vmem()] * 7,
        out_specs=[vmem()] * 2,
        compiler_params=params,
        cost_estimate=pl.CostEstimate(flops=10**9, bytes_accessed=2**22, transcendentals=0),
        name="compress",
    )(take(x), norm_gain[None], down_latent, rotary_proj, latent_gain[None], take(cs), take(sn))
    parts = [lax.all_gather(part, ("sp", "tp"), axis=0, tiled=True) for part in (g0, g1)]

    qw, kv, q = pl.pallas_call(
        functools.partial(project_kernel, block=256, heads=heads),
        out_shape=(
            jax.ShapeDtypeStruct((rows, heads_dev * HD), BF),
            jax.ShapeDtypeStruct((rows, 2 * kv_dev * HD), BF),
            jax.ShapeDtypeStruct((heads, rows, LANES), BF),
        ),
        in_specs=[vmem()] * 10,
        out_specs=[vmem()] * 3,
        compiler_params=params,
        cost_estimate=pl.CostEstimate(flops=10**10, bytes_accessed=2**23, transcendentals=0),
        name="project",
    )(x, norm_gain[None], window_query, window_key, window_value, down_query,
      query_gain[None], up_query, cs, sn)

    up = [(i, i + 1) for i in range(sp - 1)]
    before = lax.ppermute(kv[rows - WINDOW:], "sp", up)
    after = lax.ppermute(kv[:WINDOW], "sp", [(j, i) for i, j in up])

    ids = lax.axis_index("tp") * heads_dev + jnp.arange(heads_dev, dtype=jnp.int32)
    slopes = jnp.exp2(-8.0 * (ids.astype(F32) + 1.0) / A_HEADS)[None]
    smem = pl.BlockSpec(memory_space=pltpu.SMEM)
    out_window = pl.pallas_call(
        functools.partial(window_kernel, kv_dev=kv_dev, group=group, sp=sp),
        out_shape=jax.ShapeDtypeStruct((rows, heads_dev * HD), BF),
        in_specs=[vmem()] * 4 + [smem] * 2,
        out_specs=vmem(),
        scratch_shapes=[pltpu.VMEM((rows + 2 * WINDOW, 2 * kv_dev * HD), BF)],
        compiler_params=pltpu.CompilerParams(vmem_limit_bytes=VMEM_LIMIT),
        cost_estimate=pl.CostEstimate(flops=2 * 10**9, bytes_accessed=2**21, transcendentals=2**21),
        name="window",
    )(qw, kv, before, after, sink_logit[None], slopes)

    total = rows * sp // 2
    ukv = jnp.concatenate([up_key, up_value], axis=1)
    state = ()
    for part, last in zip(parts, (False, True)):
        state = (pl.pallas_call(
            functools.partial(latent_kernel, heads=heads, qb=256, kc=1024, eb=512, last=last),
            out_shape=jax.ShapeDtypeStruct((heads, rows, VD if last else LANES), BF if last else F32),
            in_specs=[vmem()] * (3 + len(state)),
            out_specs=vmem(),
            scratch_shapes=[
                pltpu.VMEM((heads, total, LANES), BF),
                pltpu.VMEM((heads, total, LANES), BF),
                pltpu.VMEM((256, total), F32),
                pltpu.VMEM((256, total), F32),
            ],
            compiler_params=params,
            cost_estimate=pl.CostEstimate(
                flops=2 * 10**10, bytes_accessed=2**23, transcendentals=2**23),
            name="latent_last" if last else "latent_first",
        )(q, part, ukv, *state),)
    out_latent = state[0].transpose(1, 0, 2).reshape(rows, heads * VD)
    chips = tp // 2
    width = window_out.shape[1]
    return pl.pallas_call(
        functools.partial(mix_kernel, chips=chips, own=own),
        out_shape=jax.ShapeDtypeStruct((own, width), BF),
        in_specs=[vmem()] * 4,
        out_specs=vmem(),
        scratch_shapes=[pltpu.VMEM((chips, own, width), BF)] * 2
        + [pltpu.VMEM((max(chips - 1, 1), own, width), BF)] * 2
        + [pltpu.SemaphoreType.DMA((chips,))] * 4,
        compiler_params=pltpu.CompilerParams(
            vmem_limit_bytes=VMEM_LIMIT, collective_id=1, has_side_effects=True),
        name="mix",
    )(out_window, out_latent, window_out, latent_out)


def solution(mesh):
    placed = (
        P("sp", "tp"), P(), P(None, "tp"), P(None, "tp"), P(None, "tp"), P("tp"), P(), P(), P(),
        P(), P(), P(None, "tp"), P(None, "tp"), P(None, "tp"), P("tp", None), P("tp", None),
    )
    return jax.shard_map(
        per_device, mesh=mesh, in_specs=placed, out_specs=P(("sp", "tp"), None), check_vma=False
    )
```
